32 devices in a mesh: sp: 8 (over z, x), dp: 4 (over y, core).
Axes of the slice: x: 2, y: 2, z: 4, core: 2. Of those that a mesh axis runs over, the one named last changes fastest.
Arguments:
- inputs: bfloat16 [1536, 2048], P('sp'), may hold values from -6 to 6
- w_query: bfloat16 [2048, 2048], P('dp'), may hold values from -0.125 to 0.125
- w_key: bfloat16 [1024, 2048], P('dp'), may hold values from -0.125 to 0.125
- w_value: bfloat16 [1024, 2048], P('dp'), may hold values from -0.125 to 0.125
- query_gain: float32 [64], replicated, may hold values from 0.6 to 7
- key_gain: float32 [64], replicated, may hold values from 0.6 to 7
- grad_out: bfloat16 [1536, 2048], P('sp', 'dp'), may hold values from -6 to 6
Outputs:
- d_inputs: bfloat16 [1536, 2048], P('sp', 'dp')
- grad_wq: float32 [2048, 2048], P('dp')
- grad_wk: float32 [1024, 2048], P('dp')
- grad_wv: float32 [1024, 2048], P('dp')
The draws below stay inside these ranges and needn't reach their ends.
All inputs are finite; a program needn't handle non-finite values.
Results may differ from the reference program's by a relative error of at most 0.019.
The reference program's roundings to bfloat16 on the way count: a program that leaves them out, or rounds other values in their place, can miss the bound.
Values may be sent and summed in bfloat16 or wider, within the bound.
No kernel may reach another device: no remote copies, remote signals or barrier semaphores. Data moves between devices by JAX's collectives and lax.ppermute only.
A program may use at most 64 MiB of HBM per device.

```python
import math
import jax
import jax.numpy as jnp
from jax import lax

D = 2048
HEAD_WIDTH = 64
QHEADS = 32
KEY_VALUE_HEADS = 16
GRID_W = 64
SEQUENCE_TOKENS = 1536
N_DP = 4


def gain_values(key):
    return jnp.exp(jax.random.uniform(key, (HEAD_WIDTH,), jnp.float32, math.log(0.6), math.log(1.6)))


def draw_query_gain(key, part):
    return gain_values(jax.random.fold_in(key, 31))


def draw_key_gain(key, part):
    return gain_values(jax.random.fold_in(key, 47))


def levels(key, shape, cuts, least, high):
    level = 1.0
    for position, blocks in cuts:
        draws = jax.random.uniform(jax.random.fold_in(jax.random.fold_in(key, 6), position), (blocks,), jnp.float32, least / len(cuts), high / len(cuts))
        level = level * jnp.repeat(jnp.exp(draws), shape[position] // blocks).reshape((-1,) + (1,) * (len(shape) - 1 - position))
    return level


def gaussian(stream_key, dims, scale, reach, split=(), kind=jnp.bfloat16):
    values = scale * jax.random.normal(stream_key, dims, jnp.float32)
    if split:
        values = values * levels(stream_key, dims, split, -0.22, 0.18)
    return jnp.clip(values, -reach, reach).astype(kind)


def setup_inputs(seed: int = 0) -> dict:
    arg_keys = jax.random.split(jax.random.key(seed), 8)
    return {
        "inputs": gaussian(arg_keys[0], (SEQUENCE_TOKENS, D), 1.0, 6.0, ((0, 8),)),
        "w_query": gaussian(arg_keys[1], (QHEADS * HEAD_WIDTH, D), D ** -0.5, 0.125, ((0, 4),)),
        "w_key": gaussian(arg_keys[2], (KEY_VALUE_HEADS * HEAD_WIDTH, D), D ** -0.5, 0.125, ((0, 4),)),
        "w_value": gaussian(arg_keys[3], (KEY_VALUE_HEADS * HEAD_WIDTH, D), D ** -0.5, 0.125, ((0, 4),)),
        "query_gain": draw_query_gain(jax.random.fold_in(arg_keys[7], 71), 0),
        "key_gain": draw_key_gain(jax.random.fold_in(arg_keys[7], 71), 0),
        "grad_out": gaussian(arg_keys[6], (SEQUENCE_TOKENS, QHEADS * HEAD_WIDTH), 1.0, 6.0, ((0, 8), (1, 4))),
    }


norm_eps = 1e-06
axial_base = 10000.0

def rotation_tables(offset, count):
    positions = offset + jnp.arange(count, dtype=jnp.int32)
    grid_rows = (positions // GRID_W).astype(jnp.float32)
    grid_cols = (positions % GRID_W).astype(jnp.float32)
    quarter = HEAD_WIDTH // 4
    freqs_axis = axial_base ** (-jnp.arange(quarter, dtype=jnp.float32) / quarter)
    angle_rows = grid_rows[:, None] * freqs_axis[None, :]
    angle_cols = grid_cols[:, None] * freqs_axis[None, :]
    cosine = jnp.concatenate([jnp.cos(angle_rows), jnp.cos(angle_rows), jnp.cos(angle_cols), jnp.cos(angle_cols)], axis=1)
    sine = jnp.concatenate([jnp.sin(angle_rows), jnp.sin(angle_rows), jnp.sin(angle_cols), jnp.sin(angle_cols)], axis=1)
    return (cosine, sine)

def quarter_turn(values):
    quarter = HEAD_WIDTH // 4
    return jnp.concatenate([-values[..., quarter:2 * quarter], values[..., :quarter], -values[..., 3 * quarter:], values[..., 2 * quarter:3 * quarter]], axis=-1)

def quarter_back(values):
    quarter = HEAD_WIDTH // 4
    return jnp.concatenate([values[..., quarter:2 * quarter], -values[..., :quarter], values[..., 3 * quarter:], -values[..., 2 * quarter:3 * quarter]], axis=-1)

def rotate(values, cosine, sine):
    return values * cosine + quarter_turn(values) * sine

def rotate_back(grads, cosine, sine):
    return grads * cosine + quarter_back(grads * sine)

def head_norm(raw):
    scale_inv = lax.rsqrt(lax.optimization_barrier(jnp.mean(raw * raw, axis=-1, keepdims=True)) + norm_eps)
    return (raw * scale_inv, scale_inv)

def head_norm_back(grads, normed, scale_inv, gain):
    scaled = grads * gain
    return scale_inv * (scaled - normed * lax.optimization_barrier(jnp.mean(scaled * normed, axis=-1, keepdims=True)))

def reference(inputs, w_query, w_key, w_value, query_gain, key_gain, grad_out):
    group = QHEADS // KEY_VALUE_HEADS
    scale = HEAD_WIDTH ** (-0.5)
    cosine, sine = rotation_tables(0, SEQUENCE_TOKENS)
    cos_wide = cosine[:, None, :]
    sin_wide = sine[:, None, :]
    q_raw = jnp.dot(inputs, w_query.T, preferred_element_type=jnp.float32).astype(jnp.bfloat16)
    k_raw = jnp.dot(inputs, w_key.T, preferred_element_type=jnp.float32).astype(jnp.bfloat16)
    v_raw = jnp.dot(inputs, w_value.T, preferred_element_type=jnp.float32).astype(jnp.bfloat16)
    q_wide = lax.optimization_barrier(q_raw).astype(jnp.float32).reshape(SEQUENCE_TOKENS, QHEADS, HEAD_WIDTH)
    k_wide = lax.optimization_barrier(k_raw).astype(jnp.float32).reshape(SEQUENCE_TOKENS, KEY_VALUE_HEADS, HEAD_WIDTH)
    q_normed, q_inv = head_norm(q_wide)
    k_normed, k_inv = head_norm(k_wide)
    q_rot = rotate(q_normed * query_gain, cos_wide, sin_wide).astype(jnp.bfloat16)
    k_rot = rotate(k_normed * key_gain, cos_wide, sin_wide).astype(jnp.bfloat16)
    query_heads = q_rot.reshape(SEQUENCE_TOKENS, KEY_VALUE_HEADS, group, HEAD_WIDTH).transpose(1, 0, 2, 3)
    gradient_heads = grad_out.reshape(SEQUENCE_TOKENS, KEY_VALUE_HEADS, group, HEAD_WIDTH).transpose(1, 0, 2, 3)
    key_heads = k_rot.transpose(1, 0, 2)
    value_heads = v_raw.reshape(SEQUENCE_TOKENS, KEY_VALUE_HEADS, HEAD_WIDTH).transpose(1, 0, 2)

    def single_key_head(operands):
        query_rot, key_rot, value_rows, grad_rows = operands
        grad_query = []
        grad_key = jnp.zeros((SEQUENCE_TOKENS, HEAD_WIDTH), jnp.float32)
        grad_value = jnp.zeros((SEQUENCE_TOKENS, HEAD_WIDTH), jnp.float32)
        for member in range(group):
            query_head = query_rot[:, member]
            grad_head = grad_rows[:, member]
            scores = jnp.dot(query_head, key_rot.T, preferred_element_type=jnp.float32) * scale
            maxima = lax.optimization_barrier(jnp.max(scores, axis=1, keepdims=True))
            log_total = maxima + jnp.log(lax.optimization_barrier(jnp.sum(jnp.exp(scores - maxima), axis=1, keepdims=True)))
            prob_exact = jnp.exp(scores - log_total)
            prob_half = prob_exact.astype(jnp.bfloat16)
            attn_rows = jnp.dot(prob_half, value_rows, preferred_element_type=jnp.float32).astype(jnp.bfloat16)
            attn_wide = lax.optimization_barrier(attn_rows).astype(jnp.float32)
            delta_rows = lax.optimization_barrier(jnp.sum(grad_head.astype(jnp.float32) * attn_wide, axis=1, keepdims=True))
            grad_value = grad_value + jnp.dot(prob_half.T, grad_head, preferred_element_type=jnp.float32)
            dprob = jnp.dot(grad_head, value_rows.T, preferred_element_type=jnp.float32)
            dscore = (prob_exact * (dprob - delta_rows)).astype(jnp.bfloat16)
            grad_query.append(jnp.dot(dscore, key_rot, preferred_element_type=jnp.float32) * scale)
            grad_key = grad_key + jnp.dot(dscore.T, query_head, preferred_element_type=jnp.float32) * scale
        return (jnp.stack(grad_query, axis=1), grad_key, grad_value)
    gradient_query_rotated, gradient_key_rotated, gradient_value_rotated = lax.map(single_key_head, (query_heads, key_heads, value_heads, gradient_heads))
    gradient_query_rotated = gradient_query_rotated.transpose(1, 0, 2, 3).reshape(SEQUENCE_TOKENS, QHEADS, HEAD_WIDTH)
    gradient_key_rotated = gradient_key_rotated.transpose(1, 0, 2)
    gradient_values = gradient_value_rotated.transpose(1, 0, 2).reshape(SEQUENCE_TOKENS, KEY_VALUE_HEADS * HEAD_WIDTH).astype(jnp.bfloat16)
    grad_q = head_norm_back(rotate_back(gradient_query_rotated, cos_wide, sin_wide), q_normed, q_inv, query_gain)
    grad_q = grad_q.reshape(SEQUENCE_TOKENS, QHEADS * HEAD_WIDTH).astype(jnp.bfloat16)
    grad_k = head_norm_back(rotate_back(gradient_key_rotated, cos_wide, sin_wide), k_normed, k_inv, key_gain)
    grad_k = grad_k.reshape(SEQUENCE_TOKENS, KEY_VALUE_HEADS * HEAD_WIDTH).astype(jnp.bfloat16)
    query_cols = QHEADS * HEAD_WIDTH // N_DP
    key_cols = KEY_VALUE_HEADS * HEAD_WIDTH // N_DP
    total = jnp.zeros((SEQUENCE_TOKENS, D), jnp.float32)
    for group_index in range(N_DP):
        q_lo = group_index * query_cols
        k_lo = group_index * key_cols
        head_part = jnp.dot(grad_q[:, q_lo:q_lo + query_cols], w_query[q_lo:q_lo + query_cols], preferred_element_type=jnp.float32)
        head_part = head_part + jnp.dot(grad_k[:, k_lo:k_lo + key_cols], w_key[k_lo:k_lo + key_cols], preferred_element_type=jnp.float32)
        head_part = head_part + jnp.dot(gradient_values[:, k_lo:k_lo + key_cols], w_value[k_lo:k_lo + key_cols], preferred_element_type=jnp.float32)
        rounded = lax.optimization_barrier(head_part.astype(jnp.bfloat16))
        total = total + rounded.astype(jnp.float32)
    d_inputs = total.astype(jnp.bfloat16)
    grad_wq = jnp.dot(grad_q.T, inputs, preferred_element_type=jnp.float32)
    grad_wk = jnp.dot(grad_k.T, inputs, preferred_element_type=jnp.float32)
    grad_wv = jnp.dot(gradient_values.T, inputs, preferred_element_type=jnp.float32)
    return (d_inputs, grad_wq, grad_wk, grad_wv)
```

```python
import jax
import jax.numpy as jnp
from jax import lax
from jax.experimental import pallas as pl
from jax.experimental.pallas import tpu as pltpu
from jax.sharding import PartitionSpec as P

HEAD_WIDTH = 64
GRID_W = 64


norm_eps = 1e-06
axial_base = 10000.0


def rotation_tables(offset, count):
    positions = offset + jnp.arange(count, dtype=jnp.int32)
    grid_rows = (positions // GRID_W).astype(jnp.float32)
    grid_cols = (positions % GRID_W).astype(jnp.float32)
    quarter = HEAD_WIDTH // 4
    freqs_axis = axial_base ** (-jnp.arange(quarter, dtype=jnp.float32) / quarter)
    angle_rows = grid_rows[:, None] * freqs_axis[None, :]
    angle_cols = grid_cols[:, None] * freqs_axis[None, :]
    cosine = jnp.concatenate(
        [jnp.cos(angle_rows), jnp.cos(angle_rows), jnp.cos(angle_cols), jnp.cos(angle_cols)], axis=1
    )
    sine = jnp.concatenate(
        [jnp.sin(angle_rows), jnp.sin(angle_rows), jnp.sin(angle_cols), jnp.sin(angle_cols)], axis=1
    )
    return (cosine, sine)


def quarter_turn(values):
    quarter = HEAD_WIDTH // 4
    return jnp.concatenate(
        [
            -values[..., quarter : 2 * quarter],
            values[..., :quarter],
            -values[..., 3 * quarter :],
            values[..., 2 * quarter : 3 * quarter],
        ],
        axis=-1,
    )


def quarter_back(values):
    quarter = HEAD_WIDTH // 4
    return jnp.concatenate(
        [
            values[..., quarter : 2 * quarter],
            -values[..., :quarter],
            values[..., 3 * quarter :],
            -values[..., 2 * quarter : 3 * quarter],
        ],
        axis=-1,
    )


def rotate(values, cosine, sine):
    return values * cosine + quarter_turn(values) * sine


def rotate_back(grads, cosine, sine):
    return grads * cosine + quarter_back(grads * sine)


def head_norm(raw):
    scale_inv = lax.rsqrt(jnp.mean(raw * raw, axis=-1, keepdims=True) + norm_eps)
    return (raw * scale_inv, scale_inv)


def head_norm_back(grads, normed, scale_inv, gain):
    scaled = grads * gain
    return scale_inv * (scaled - normed * jnp.mean(scaled * normed, axis=-1, keepdims=True))


def body(inputs, w_query, w_key, w_value, query_gain, key_gain, grad_out):
    tok_rows = inputs.shape[0]
    local_query = w_query.shape[0] // HEAD_WIDTH
    local_keys = w_key.shape[0] // HEAD_WIDTH
    group = local_query // local_keys
    key_width = local_keys * HEAD_WIDTH
    scale = HEAD_WIDTH ** (-0.5)
    contract = (((1,), (1,)), ((), ()))
    leading = (((0,), (0,)), ((), ()))
    offset = lax.axis_index("sp") * tok_rows
    cosine, sine = rotation_tables(offset, tok_rows)
    cos_wide = cosine[:, None, :]
    sin_wide = sine[:, None, :]
    q_raw = lax.dot_general(inputs, w_query, contract, preferred_element_type=jnp.float32).astype(
        jnp.bfloat16
    )
    w_pair = jnp.concatenate([w_key, w_value], axis=0)
    kv_raw = lax.dot_general(inputs, w_pair, contract, preferred_element_type=jnp.float32).astype(
        jnp.bfloat16
    )
    q_wide = (
        lax.optimization_barrier(q_raw)
        .astype(jnp.float32)
        .reshape(tok_rows, local_query, HEAD_WIDTH)
    )
    k_wide = (
        lax.optimization_barrier(kv_raw[:, :key_width])
        .astype(jnp.float32)
        .reshape(tok_rows, local_keys, HEAD_WIDTH)
    )
    q_normed, q_inv = head_norm(q_wide)
    k_normed, k_inv = head_norm(k_wide)
    q_rot = rotate(q_normed * query_gain, cos_wide, sin_wide).astype(jnp.bfloat16)
    k_rot = rotate(k_normed * key_gain, cos_wide, sin_wide).astype(jnp.bfloat16)
    kv_rot = jnp.concatenate([k_rot.reshape(tok_rows, key_width), kv_raw[:, key_width:]], axis=1)
    kv_every = lax.all_gather(kv_rot, "sp", axis=0, tiled=True)
    seq_rows = kv_every.shape[0]
    keys_every = kv_every[:, :key_width]
    values_every = kv_every[:, key_width:]
    grad_query = []
    log_totals = []
    deltas = []
    key_terms = [jnp.zeros((seq_rows, HEAD_WIDTH), jnp.float32) for slot in range(local_keys)]
    value_terms = [jnp.zeros((seq_rows, HEAD_WIDTH), jnp.float32) for slot in range(local_keys)]
    for member in range(local_query):
        kv_index = member // group
        query_head = q_rot[:, member, :]
        key_head = keys_every[:, kv_index * HEAD_WIDTH : (kv_index + 1) * HEAD_WIDTH]
        value_head = values_every[:, kv_index * HEAD_WIDTH : (kv_index + 1) * HEAD_WIDTH]
        grad_head = grad_out[:, member * HEAD_WIDTH : (member + 1) * HEAD_WIDTH]
        scores = (
            lax.dot_general(query_head, key_head, contract, preferred_element_type=jnp.float32)
            * scale
        )
        maxima = jnp.max(scores, axis=1, keepdims=True)
        log_total = maxima + jnp.log(jnp.sum(jnp.exp(scores - maxima), axis=1, keepdims=True))
        prob_exact = jnp.exp(scores - log_total)
        prob_half = prob_exact.astype(jnp.bfloat16)
        attn_rows = jnp.dot(prob_half, value_head, preferred_element_type=jnp.float32).astype(
            jnp.bfloat16
        )
        attn_wide = lax.optimization_barrier(attn_rows).astype(jnp.float32)
        delta_rows = jnp.sum(grad_head.astype(jnp.float32) * attn_wide, axis=1, keepdims=True)
        dprob = lax.dot_general(grad_head, value_head, contract, preferred_element_type=jnp.float32)
        dscore = (prob_exact * (dprob - delta_rows)).astype(jnp.bfloat16)
        grad_query.append(jnp.dot(dscore, key_head, preferred_element_type=jnp.float32) * scale)
        log_totals.append(log_total)
        deltas.append(delta_rows)
        value_terms[kv_index] = value_terms[kv_index] + lax.dot_general(
            prob_half, grad_head, leading, preferred_element_type=jnp.float32
        )
        key_terms[kv_index] = (
            key_terms[kv_index]
            + lax.dot_general(dscore, query_head, leading, preferred_element_type=jnp.float32)
            * scale
        )
    gradient_query_rotated = jnp.stack(grad_query, axis=1)
    partial_sums = jnp.concatenate(key_terms + value_terms, axis=1)
    own_grads = lax.psum_scatter(partial_sums, "sp", scatter_dimension=0, tiled=True)
    gradient_key_rotated = own_grads[:, :key_width].reshape(tok_rows, local_keys, HEAD_WIDTH)
    grad_q = head_norm_back(
        rotate_back(gradient_query_rotated, cos_wide, sin_wide), q_normed, q_inv, query_gain
    )
    grad_q = grad_q.reshape(tok_rows, local_query * HEAD_WIDTH).astype(jnp.bfloat16)
    grad_k = head_norm_back(
        rotate_back(gradient_key_rotated, cos_wide, sin_wide), k_normed, k_inv, key_gain
    )
    grad_kv = jnp.concatenate(
        [
            grad_k.reshape(tok_rows, key_width).astype(jnp.bfloat16),
            own_grads[:, key_width:].astype(jnp.bfloat16),
        ],
        axis=1,
    )
    head_part = jnp.dot(grad_q, w_query, preferred_element_type=jnp.float32)
    head_part = head_part + jnp.dot(grad_kv, w_pair, preferred_element_type=jnp.float32)
    d_inputs = lax.psum_scatter(
        head_part.astype(jnp.bfloat16), "dp", scatter_dimension=1, tiled=True
    )
    grad_wq = lax.dot_general(grad_q, inputs, leading, preferred_element_type=jnp.float32)
    grad_wkv = lax.dot_general(grad_kv, inputs, leading, preferred_element_type=jnp.float32)
    grad_wq, grad_wkv = lax.psum((grad_wq, grad_wkv), "sp")
    return (d_inputs, grad_wq, grad_wkv[:key_width], grad_wkv[key_width:])


def ring_order(index, count):
    return jnp.where(index < count // 2, 2 * index, 2 * (count - 1 - index) + 1)


def ring_place(device, count):
    return jnp.where(device % 2 == 0, device // 2, count - 1 - device // 2)


def ring_steps(block, me, count):
    order = list(range(0, count, 2)) + list(range(count - 1, 0, -2))
    ahead = [(order[i], order[(i + 1) % count]) for i in range(count)]
    behind = [(b, a) for a, b in ahead]
    place = ring_place(me, count)
    yield me, block
    first = second = block
    for step in range(1, count // 2 + 1):
        first = lax.ppermute(first, "sp", ahead)
        if step < count // 2:
            second = lax.ppermute(second, "sp", behind)
        yield ring_order((place - step) % count, count), first
        if step < count // 2:
            yield ring_order((place + step) % count, count), second


def dot_nt(a, b):
    return lax.dot_general(a, b, (((1,), (1,)), ((), ())), preferred_element_type=jnp.float32)


def dot_nn(a, b):
    return jnp.dot(a, b, preferred_element_type=jnp.float32)


def project_kernel(x_ref, wq_ref, wk_ref, wv_ref, grad_ref, out_ref):
    heads = out_ref.shape[0]
    group = wq_ref.shape[0] // wk_ref.shape[0]
    x = x_ref[...]
    q = dot_nt(x, wq_ref[...]).astype(jnp.bfloat16)
    k = dot_nt(x, wk_ref[...]).astype(jnp.bfloat16)
    v = dot_nt(x, wv_ref[...]).astype(jnp.bfloat16)
    grad = grad_ref[...]

    def head(values, index):
        return values[:, index * HEAD_WIDTH : (index + 1) * HEAD_WIDTH]

    for h in range(heads):
        out_ref[h] = jnp.concatenate(
            [head(q, h), head(k, h // group), head(grad, h), head(v, h // group)], axis=1
        )


def turn_rows(values):
    q = HEAD_WIDTH // 4
    return jnp.concatenate(
        [-values[q : 2 * q], values[:q], -values[3 * q :], values[2 * q : 3 * q]], axis=0
    )


def back_rows(values):
    q = HEAD_WIDTH // 4
    return jnp.concatenate(
        [values[q : 2 * q], -values[:q], values[3 * q :], -values[2 * q : 3 * q]], axis=0
    )


def norm_rows(raw):
    inv = lax.rsqrt(jnp.mean(raw * raw, axis=0, keepdims=True) + norm_eps)
    return raw * inv, inv


def norm_back_rows(grads, normed, inv, gain):
    scaled = grads * gain
    return inv * (scaled - normed * jnp.mean(scaled * normed, axis=0, keepdims=True))


def attention_kernel(
    x_ref, cos_ref, sin_ref, qg_ref, kg_ref, gq_ref, dkv_ref, kn_ref, ki_ref, q_s, go_s, k_s, qn_s, qi_s, dq_s
):
    width = HEAD_WIDTH
    seq = x_ref.shape[0]
    scale = width ** (-0.5)
    xt = x_ref[...].T
    cosine = cos_ref[...]
    sine = sin_ref[...]
    qn, qi = norm_rows(xt[:width].astype(jnp.float32))
    kn, ki = norm_rows(xt[width : 2 * width].astype(jnp.float32))
    qn_s[...] = qn
    qi_s[...] = qi
    kn_ref[...] = kn
    ki_ref[...] = jnp.broadcast_to(ki, ki_ref.shape)
    qg = qn * qg_ref[...]
    kg = kn * kg_ref[...]
    q_s[...] = (qg * cosine + turn_rows(qg) * sine).astype(jnp.bfloat16)
    kt = (kg * cosine + turn_rows(kg) * sine).astype(jnp.bfloat16)
    go_s[...] = xt[2 * width : 3 * width]
    vt = xt[3 * width :]
    k_s[:width] = kt
    k_s[width:] = vt
    rows = k_s[...].T
    k_rows = rows[:, :width]
    v_rows = rows[:, width:]
    dkv_ref[...] = jnp.zeros_like(dkv_ref)
    block = 256

    def step(i, carry):
        at = pl.ds(pl.multiple_of(i * block, block), block)
        q = q_s[:, at]
        go = go_s[:, at]
        scores = dot_nn(k_rows, q) * scale
        maxima = jnp.max(scores, axis=0, keepdims=True)
        weights = jnp.exp(scores - maxima)
        prob = weights * (1.0 / jnp.sum(weights, axis=0, keepdims=True))
        half = prob.astype(jnp.bfloat16)
        attn = dot_nn(vt, half).astype(jnp.bfloat16)
        delta = jnp.sum(go.astype(jnp.float32) * attn.astype(jnp.float32), axis=0, keepdims=True)
        dprob = dot_nn(v_rows, go)
        dscore = (prob * (dprob - delta)).astype(jnp.bfloat16)
        dq_s[:, at] = dot_nn(kt, dscore) * scale
        dkv_ref[:width] += dot_nt(q, dscore) * scale
        dkv_ref[width:] += dot_nt(go, half)
        return carry

    lax.fori_loop(0, seq // block, step, 0)
    dq = dq_s[...]
    back = dq * cosine + back_rows(dq * sine)
    gq_ref[...] = norm_back_rows(back, qn_s[...], qi_s[...], qg_ref[...]).astype(jnp.bfloat16)


def key_kernel(part_ref, own_ref, other_ref, kn_ref, ki_ref, cos_ref, sin_ref, kg_ref, out_ref):
    width = HEAD_WIDTH
    total = own_ref[...] + other_ref[...]
    dk = total[:width]
    back = dk * cos_ref[...] + back_rows(dk * sin_ref[...])
    out_ref[:width] = norm_back_rows(back, kn_ref[...], ki_ref[:1], kg_ref[...]).astype(jnp.bfloat16)
    out_ref[width:] = total[width:].astype(jnp.bfloat16)


def head_body(inputs, w_query, w_key, w_value, query_gain, key_gain, grad_out):
    count = lax.axis_size("sp")
    cores = lax.axis_size("dp")
    tok, width = inputs.shape
    seq = tok * count
    heads = w_query.shape[0] // HEAD_WIDTH
    keys = w_key.shape[0] // HEAD_WIDTH
    half_w = width // 2
    half_s = seq // 2
    me = lax.axis_index("sp")
    side = lax.axis_index("dp") % 2
    bf16, f32 = jnp.bfloat16, jnp.float32
    struct = jax.ShapeDtypeStruct

    blocks = pl.pallas_call(
        project_kernel, out_shape=struct((heads, tok, 4 * HEAD_WIDTH), bf16), name="project"
    )(inputs, w_query, w_key, w_value, grad_out)
    gathered = lax.all_to_all(
        blocks.reshape(heads * tok, 4 * HEAD_WIDTH), "sp", split_axis=0, concat_axis=0, tiled=True
    )

    mine = lax.dynamic_slice(inputs, (0, side * half_w), (tok, half_w))
    x_half = jnp.zeros((seq, half_w), bf16)
    for source, piece in ring_steps(mine, me, count):
        x_half = lax.dynamic_update_slice(x_half, piece, (source * tok, 0))
    x_other = lax.ppermute(x_half, "dp", [(i, i ^ 1) for i in range(cores)])

    cosine, sine = rotation_tables(0, seq)
    cosine, sine = cosine.T, sine.T
    qg = query_gain[:, None]
    kg = key_gain[:, None]
    vmem = pltpu.VMEM
    gq, dkv, kn, ki = pl.pallas_call(
        attention_kernel,
        out_shape=(
            struct((HEAD_WIDTH, seq), bf16),
            struct((2 * HEAD_WIDTH, seq), f32),
            struct((HEAD_WIDTH, seq), f32),
            struct((8, seq), f32),
        ),
        scratch_shapes=[
            vmem((HEAD_WIDTH, seq), bf16),
            vmem((HEAD_WIDTH, seq), bf16),
            vmem((2 * HEAD_WIDTH, seq), bf16),
            vmem((HEAD_WIDTH, seq), f32),
            vmem((1, seq), f32),
            vmem((HEAD_WIDTH, seq), f32),
        ],
        name="attention",
    )(gathered, cosine, sine, qg, kg)

    part = me % 2
    away = lax.dynamic_slice(dkv, (0, (1 - part) * half_s), (2 * HEAD_WIDTH, half_s))
    other = lax.ppermute(away, "sp", [(i, i ^ 1) for i in range(count)])

    def at_part(rows):
        return pl.BlockSpec((rows, half_s), lambda i, p: (0, p[0]))

    def whole(rows, cols):
        return pl.BlockSpec((rows, cols), lambda i, p: (0, 0))

    gkv = pl.pallas_call(
        key_kernel,
        out_shape=struct((2 * HEAD_WIDTH, half_s), bf16),
        grid_spec=pltpu.PrefetchScalarGridSpec(
            num_scalar_prefetch=1,
            grid=(1,),
            in_specs=[
                at_part(2 * HEAD_WIDTH),
                whole(2 * HEAD_WIDTH, half_s),
                at_part(HEAD_WIDTH),
                at_part(8),
                at_part(HEAD_WIDTH),
                at_part(HEAD_WIDTH),
                whole(HEAD_WIDTH, 1),
            ],
            out_specs=whole(2 * HEAD_WIDTH, half_s),
        ),
        name="keys",
    )(part.reshape(1).astype(jnp.int32), dkv, other, kn, ki, cosine, sine, kg)

    gq_every = jnp.zeros((heads * HEAD_WIDTH, seq), bf16)
    for source, piece in ring_steps(gq, me, count):
        gq_every = lax.dynamic_update_slice(gq_every, piece, (source * HEAD_WIDTH, 0))
    gk_every = jnp.zeros((keys * HEAD_WIDTH, seq), bf16)
    gv_every = jnp.zeros((keys * HEAD_WIDTH, seq), bf16)
    for source, piece in ring_steps(gkv, me, count):
        where = (source // 2 * HEAD_WIDTH, source % 2 * half_s)
        gk_every = lax.dynamic_update_slice(gk_every, piece[:HEAD_WIDTH], where)
        gv_every = lax.dynamic_update_slice(gv_every, piece[HEAD_WIDTH:], where)

    x_every = jnp.zeros((seq, width), bf16)
    x_every = lax.dynamic_update_slice(x_every, x_half, (0, side * half_w))
    x_every = lax.dynamic_update_slice(x_every, x_other, (0, (1 - side) * half_w))

    leading = (((0,), (0,)), ((), ()))

    def share(grads, weight):
        own = lax.dynamic_slice(grads, (0, me * tok), (grads.shape[0], tok))
        return lax.dot_general(own, weight, leading, preferred_element_type=f32)

    head_part = share(gq_every, w_query) + share(gk_every, w_key) + share(gv_every, w_value)
    shares = lax.all_to_all(
        head_part.astype(bf16), "dp", split_axis=1, concat_axis=0, tiled=True
    ).reshape(cores, tok, width // cores)
    d_inputs = jnp.sum(shares.astype(f32), axis=0).astype(bf16)
    return (
        d_inputs,
        dot_nn(gq_every, x_every),
        dot_nn(gk_every, x_every),
        dot_nn(gv_every, x_every),
    )


def choose(inputs, w_query, w_key, w_value, query_gain, key_gain, grad_out):
    count = lax.axis_size("sp")
    cores = lax.axis_size("dp")
    heads = w_query.shape[0] // HEAD_WIDTH
    keys = w_key.shape[0] // HEAD_WIDTH
    seq = inputs.shape[0] * count
    fits = heads == count and heads == 2 * keys and cores % 2 == 0 and seq % 256 == 0
    run = head_body if fits else body
    return run(inputs, w_query, w_key, w_value, query_gain, key_gain, grad_out)


def solution(mesh):
    return jax.shard_map(
        choose,
        mesh=mesh,
        in_specs=(
            P("sp", None),
            P("dp", None),
            P("dp", None),
            P("dp", None),
            P(),
            P(),
            P("sp", "dp"),
        ),
        out_specs=(P("sp", "dp"), P("dp", None), P("dp", None), P("dp", None)),
        check_vma=False,
    )
```
